32 devices in a mesh: sp: 4 (over z), fs: 4 (over y, x), tp: 2 (over core).
Axes of the slice: x: 2, y: 2, z: 4, core: 2. Of those that a mesh axis runs over, the one named last changes fastest.
Arguments:
- tokens: bfloat16 [8, 1536, 2048], P('fs', ('sp', 'tp')), may hold values from -6 to 6
- norm_gain: float32 [2048], replicated, may hold values from 0.1 to 1.9
- chain_entry: bfloat16 [2048, 2048], P(('sp', 'fs'), 'tp'), may hold values from -0.125 to 0.125
- pool_entry: bfloat16 [2048, 2048], P(('sp', 'fs'), 'tp'), may hold values from -0.125 to 0.125
- conv_taps: bfloat16 [4, 2048], P(None, 'tp'), may hold values from -3 to 3
- recur_gate: bfloat16 [8, 256, 256], P('tp'), may hold values from -0.375 to 0.375
- input_gate: bfloat16 [8, 256, 256], P('tp'), may hold values from -0.375 to 0.375
- decay_log: float32 [2048], P('tp'), may hold values from -9 to 5
- decay_shift: float32 [8, 1536, 2048], P('fs', 'sp', 'tp'), may hold values from -1 to 0
- start_state: float32 [8, 2048], P('fs', 'tp'), may hold values from -6 to 6
- pool_mix: bfloat16 [8, 256, 256], P('tp'), may hold values from -0.375 to 0.375
- pool_scale: float32 [2048], P('tp'), may hold values from 0.1 to 1.9
- chain_exit: bfloat16 [2048, 2048], P('tp', ('sp', 'fs')), may hold values from -0.09375 to 0.09375
- pool_exit: bfloat16 [2048, 2048], P('tp', ('sp', 'fs')), may hold values from -0.09375 to 0.09375
Outputs:
- mixed_rows: bfloat16 [8, 1536, 2048], P('fs', ('sp', 'tp'))
The draws below stay inside these ranges and needn't reach their ends.
All inputs are finite; a program needn't handle non-finite values.
Results may differ from the reference program's by a relative error of at most 0.01.
Values may be sent and summed in bfloat16 or wider, within the bound.
A program may use at most 128 MiB of HBM per device.

```python
import math
import jax
import jax.numpy as jnp
from jax import lax

D = 2048
HEAD = 256
CHAIN_HEADS = 8
POOL_GROUPS = 8
CONV_TAPS = 4
POOL_SPAN = 16
TOK_DEV = 384
CHAIN_WIDTH = 2048
POOL_WIDTH = 2048
LEN = 1536
SEQS = 8


def draw_decay_log(key, part):
    inner = jax.random.fold_in(key, 7)
    return jax.random.uniform(inner, (CHAIN_WIDTH,), jnp.float32, -9.0, 5.0)


def draw_decay_shift(key, part):
    inner = jax.random.fold_in(key, 11)
    first_key, second_key, third_key, fourth_key, fifth_key, sixth_key, seventh_key = jax.random.split(inner, 7)
    block_span = TOK_DEV // 4
    block_total = SEQS * LEN // block_span
    slowness = jnp.exp(jax.random.uniform(first_key, (block_total, 1, CHAIN_WIDTH), jnp.float32, math.log(0.1), math.log(0.8)))
    jitter = jax.random.uniform(second_key, (block_total, block_span, CHAIN_WIDTH), jnp.float32, 0.5, 1.5)
    fast_share = 0.5
    fast_pick = jax.random.uniform(fifth_key, (CHAIN_WIDTH,), jnp.float32) < fast_share
    fast_rate = jnp.exp(jax.random.uniform(sixth_key, (CHAIN_WIDTH,), jnp.float32, math.log(0.012), math.log(0.035)))
    fast_boost = jnp.exp(jax.random.uniform(seventh_key, (block_total, 1, CHAIN_WIDTH), jnp.float32, math.log(0.6), math.log(1.6)))
    rate = slowness / LEN + jnp.where(fast_pick, fast_rate, 0.0)[None, None, :] * fast_boost
    steady = -(rate * jitter).reshape(SEQS, LEN, CHAIN_WIDTH)
    places = jax.random.randint(third_key, (SEQS, 4), 0, LEN)
    struck = jnp.any(jnp.arange(LEN)[None, :, None] == places[:, None, :], axis=2)
    depth = jax.random.uniform(fourth_key, (SEQS, LEN, CHAIN_WIDTH), jnp.float32, -0.7, -0.2)
    return steady + jnp.where(struck[:, :, None], depth, 0.0)


def steps_of(stream_key, extent, pieces, least, high):
    level, own = 1.0, jax.random.fold_in(stream_key, 6)
    for dim, shards_of in pieces:
        heights = jnp.exp(jax.random.uniform(jax.random.fold_in(own, dim), (shards_of,), jnp.float32, least / len(pieces), high / len(pieces)))
        level = level * jnp.repeat(heights, extent[dim] // shards_of).reshape([-1 if axis == dim else 1 for axis in range(len(extent))])
    return level


def scatter_about(stream_key, dims, width, reach, pieces=(), kind=jnp.bfloat16):
    array = width * jax.random.normal(stream_key, dims, jnp.float32)
    if pieces:
        array = array * steps_of(stream_key, dims, pieces, -0.22, 0.18)
    return jnp.clip(array, -reach, reach).astype(kind)


def setup_inputs(seed: int = 0) -> dict:
    seeds = jax.random.split(jax.random.key(seed), 15)
    return {
        "tokens": scatter_about(seeds[0], (SEQS, LEN, D), 1.0, 6.0, ((0, 4), (1, 8))),
        "norm_gain": jnp.clip(1.0 + 0.18 * jax.random.normal(seeds[1], (D,), jnp.float32), 0.1, 1.9),
        "chain_entry": scatter_about(seeds[2], (D, CHAIN_WIDTH), D ** -0.5, 0.125, ((0, 16), (1, 2))),
        "pool_entry": scatter_about(seeds[3], (D, POOL_WIDTH), D ** -0.5, 0.125, ((0, 16), (1, 2))),
        "conv_taps": scatter_about(seeds[4], (CONV_TAPS, CHAIN_WIDTH), CONV_TAPS ** -0.5, 3.0, ((1, 2),)),
        "recur_gate": scatter_about(seeds[5], (CHAIN_HEADS, HEAD, HEAD), HEAD ** -0.5, 0.375, ((0, 2),)),
        "input_gate": scatter_about(seeds[6], (CHAIN_HEADS, HEAD, HEAD), HEAD ** -0.5, 0.375, ((0, 2),)),
        "decay_log": draw_decay_log(jax.random.fold_in(seeds[14], 71), 0),
        "decay_shift": draw_decay_shift(jax.random.fold_in(seeds[14], 71), 0),
        "start_state": scatter_about(seeds[9], (SEQS, CHAIN_WIDTH), 1.0, 6.0, ((0, 4), (1, 2)), jnp.float32),
        "pool_mix": scatter_about(seeds[10], (POOL_GROUPS, HEAD, HEAD), HEAD ** -0.5, 0.375, ((0, 2),)),
        "pool_scale": jnp.clip(1.0 + 0.18 * jax.random.normal(seeds[11], (POOL_WIDTH,), jnp.float32), 0.1, 1.9),
        "chain_exit": scatter_about(seeds[12], (CHAIN_WIDTH, D), (CHAIN_WIDTH + POOL_WIDTH) ** -0.5, 0.09375, ((0, 2), (1, 16))),
        "pool_exit": scatter_about(seeds[13], (POOL_WIDTH, D), (CHAIN_WIDTH + POOL_WIDTH) ** -0.5, 0.09375, ((0, 2), (1, 16))),
    }


NORM_EPSILON = 1e-06
RECUR_SCALE = 8.0

def block_map(values, weight):
    row_total = values.shape[0]
    groups, block_width, _ = weight.shape
    blocks = values.astype(jnp.float32).reshape(row_total, groups, block_width)
    mapped = jnp.einsum('sgi,gij->sgj', blocks, weight.astype(jnp.float32))
    return mapped.reshape(row_total, groups * block_width)

def combine(earlier, latter):
    return (earlier[0] * latter[0], latter[0] * earlier[1] + latter[1])

def trailing(padded, row_total, window_id):
    sum_two = padded[1:] + padded[:-1]
    sum_four = sum_two[2:] + sum_two[:-2]
    sum_eight = sum_four[4:] + sum_four[:-4]
    sixteen = sum_eight[8:] + sum_eight[:-8]
    return jnp.where(window_id == 0, sum_two[-row_total:], jnp.where(window_id == 1, sum_four[-row_total:], jnp.where(window_id == 2, sum_eight[-row_total:], sixteen[-row_total:])))

def reference(tokens, norm_gain, chain_entry, pool_entry, conv_taps, recur_gate, input_gate, decay_log, decay_shift, start_state, pool_mix, pool_scale, chain_exit, pool_exit):
    channel = jnp.arange(POOL_WIDTH, dtype=jnp.int32) // HEAD
    window_id = (channel % 4)[None, :]
    window = jnp.power(2.0, (window_id + 1).astype(jnp.float32))
    position = jnp.arange(LEN, dtype=jnp.float32)[:, None]
    counts = jnp.minimum(position + 1.0, window)
    decay_rate = jnp.exp(decay_log) / LEN

    def one_sequence(inputs):
        values, shift_rows, begin_state = inputs
        widened = values.astype(jnp.float32)
        normed = (widened * lax.rsqrt(lax.optimization_barrier(jnp.mean(widened * widened, axis=-1, keepdims=True)) + NORM_EPSILON) * norm_gain.astype(jnp.float32)).astype(jnp.bfloat16)
        chain_input = jnp.dot(normed, chain_entry, preferred_element_type=jnp.float32).astype(jnp.bfloat16)
        pool_input = jnp.dot(normed, pool_entry, preferred_element_type=jnp.float32).astype(jnp.bfloat16)
        padded = jnp.pad(chain_input.astype(jnp.float32), ((CONV_TAPS - 1, 0), (0, 0)))
        conv_out = jnp.zeros((LEN, CHAIN_WIDTH), jnp.float32)
        for offset in range(CONV_TAPS):
            conv_out = conv_out + padded[offset:offset + LEN] * conv_taps[offset].astype(jnp.float32)
        conv_out = conv_out.astype(jnp.bfloat16)
        gate_recur = jax.nn.sigmoid(block_map(conv_out, recur_gate))
        gate_input = jax.nn.sigmoid(block_map(conv_out, input_gate))
        log_decay = -RECUR_SCALE * gate_recur * decay_rate + shift_rows
        decay_factor = jnp.exp(log_decay)
        drive_term = jnp.sqrt(-jnp.expm1(2.0 * log_decay)) * gate_input * conv_out.astype(jnp.float32)
        drive_term = drive_term.at[0].add(decay_factor[0] * begin_state)
        state = lax.associative_scan(combine, (decay_factor, drive_term), axis=0)[1]
        recurrent = state.astype(jnp.bfloat16)
        pool_pad = jnp.pad(pool_input.astype(jnp.float32), ((POOL_SPAN - 1, 0), (0, 0)))
        trail_sum = trailing(pool_pad, LEN, window_id)
        pool_diff = (trail_sum / counts - pool_input.astype(jnp.float32)).astype(jnp.bfloat16)
        pooled = (block_map(pool_diff, pool_mix) * pool_scale.astype(jnp.float32)).astype(jnp.bfloat16)
        mixed_rows = jnp.dot(recurrent, chain_exit, preferred_element_type=jnp.float32) + jnp.dot(pooled, pool_exit, preferred_element_type=jnp.float32)
        return mixed_rows.astype(jnp.bfloat16)
    return lax.map(one_sequence, (tokens, decay_shift, start_state))
```

```python
import functools

import jax
import jax.numpy as jnp
from jax import lax
from jax.experimental import pallas as pl
from jax.experimental.pallas import tpu as pltpu
from jax.sharding import PartitionSpec as P

MESH = pl.DeviceIdType.MESH
NORM_EPSILON = 1e-06
RECUR_SCALE = 8.0
HALO = 16
COLS = 256
ROWS = 64
F32 = jnp.float32
BF16 = jnp.bfloat16


def neg_expm1(x):
    y = -x
    poly = 1.0 - y * (1.0 / 9.0)
    for k in range(8, 1, -1):
        poly = 1.0 - y * (1.0 / k) * poly
    return jnp.where(y < 0.5, y * poly, 1.0 - jnp.exp(x))


def kernel(
    n, m,
    tokens, gain, chain_entry, pool_entry, taps, rgate, igate, dlog, shift_hbm, start,
    pmix, pscale, chain_exit, pool_exit,
    out,
    w0, w1, w2, w3, raw, normed, cbuf, pbuf, shift, rg, ig, pm,
    convb, zr, zi, cum_a, cum_b, rec, pooled, my_ab, all_ab, ent, acc, sendbuf, recvbuf,
    s1, r1, s2, r2, loc, nsem, hsem_s, hsem_r, ab_s, ab_r, out_s, out_r,
):
    sp, fs, tp = lax.axis_index("sp"), lax.axis_index("fs"), lax.axis_index("tp")
    shards = (chain_entry, pool_entry, chain_exit, pool_exit)
    bufs = (w0, w1, w2, w3)
    seqs, half_rows, width = raw.shape
    rows = 2 * half_rows
    chans = cbuf.shape[2]
    nb = chans // COLS
    far = m // 2
    full = (m - 1) // 2

    def ring(i):
        return i + (i // 2) * (5 - 2 * i) if m == 4 else i

    pos = ring(fs)
    right, left = ring((pos + 1) % m), ring((pos + m - 1) % m)

    barrier = pltpu.get_barrier_semaphore()
    greet = [{"sp": (sp + k) % n} for k in range(1, n)] + [{"tp": 1 - tp}]
    if m > 1:
        greet += [{"fs": right}, {"fs": left}]
    for device in greet:
        pl.semaphore_signal(barrier, inc=1, device_id=device, device_id_type=MESH)

    def region(w, p, q, part=None):
        block = shards[w].shape[0]
        at = (((sp + p) % n) * m + ring((pos + q + m) % m)) * block
        if part is None:
            return bufs[w].at[pl.ds(pl.multiple_of(at, block), block)]
        half = block // 2
        return bufs[w].at[pl.ds(pl.multiple_of(at + part * half, half), half)]

    started = []

    def launch(copy):
        copy.start()
        started.append(copy)

    def first(w, k):
        return pltpu.make_async_remote_copy(
            src_ref=shards[w], dst_ref=region(w, 0, 0), send_sem=s1.at[w * n + k],
            recv_sem=r1.at[w * n + n - k], device_id={"sp": (sp + k) % n}, device_id_type=MESH)

    def first_wait(w, p):
        pltpu.make_async_remote_copy(
            src_ref=shards[w], dst_ref=region(w, p, 0), send_sem=s1.at[w * n + p],
            recv_sem=r1.at[w * n + p], device_id={"sp": (sp + p) % n},
            device_id_type=MESH).wait_recv()

    def second(w, p, way, d):
        q = -d if way == 0 else d
        part = way if (m % 2 == 0 and d + 1 == far) else None
        if p == 0 and d == 0:
            src = shards[w]
            if part is not None:
                half = shards[w].shape[0] // 2
                src = src.at[pl.ds(part * half, half)]
        else:
            src = region(w, p, q, part)
        at = ((w * n + p) * 2 + way) * max(far, 1) + d
        return pltpu.make_async_remote_copy(
            src_ref=src, dst_ref=region(w, p, q, part), send_sem=s2.at[at], recv_sem=r2.at[at],
            device_id={"fs": right if way == 0 else left}, device_id_type=MESH)

    def second_wait(w, p, way, d):
        q = -d if way == 0 else d
        part = way if (m % 2 == 0 and d == far) else None
        at = ((w * n + p) * 2 + way) * max(far, 1) + d - 1
        ref = region(w, p, q, part)
        pltpu.make_async_remote_copy(
            src_ref=ref, dst_ref=ref, send_sem=s2.at[at], recv_sem=r2.at[at],
            device_id={"fs": right if way == 0 else left}, device_id_type=MESH).wait_recv()

    def second_all(w, p):
        if far >= 1:
            for way in (0, 1):
                launch(second(w, p, way, 0))

    def forward(w, p):
        for d in range(1, far):
            for way in (0, 1):
                second_wait(w, p, way, d)
                launch(second(w, p, way, d))

    def last_wait(w, p):
        if far >= 1:
            for way in (0, 1):
                second_wait(w, p, way, far)

    local = [
        pltpu.make_async_copy(tokens, raw, loc.at[0]),
        pltpu.make_async_copy(shift_hbm, shift, loc.at[1]),
        pltpu.make_async_copy(rgate, rg, loc.at[2]),
        pltpu.make_async_copy(igate, ig, loc.at[3]),
        pltpu.make_async_copy(pmix, pm, loc.at[4]),
    ] + [pltpu.make_async_copy(shards[w], region(w, 0, 0), loc.at[5 + w]) for w in range(4)]
    for copy in local:
        copy.start()

    pl.semaphore_wait(barrier, len(greet))
    order = sorted(range(1, n), key=lambda p: min(p, n - p))
    for w in (0, 1):
        second_all(w, 0)
        for k in order:
            launch(first(w, k))

    local[0].wait()
    mine = tp * half_rows

    def norm_step(i, c):
        s, r = i // (half_rows // ROWS), (i % (half_rows // ROWS)) * ROWS
        x = raw[s, pl.ds(pl.multiple_of(r, ROWS), ROWS), :].astype(F32)
        scale = lax.rsqrt(jnp.mean(x * x, axis=-1, keepdims=True) + NORM_EPSILON)
        normed[s, pl.ds(pl.multiple_of(mine + r, ROWS), ROWS), :] = (
            x * scale * gain[...]).astype(BF16)
        return c

    lax.fori_loop(0, seqs * (half_rows // ROWS), norm_step, 0)

    def normed_copy(owner):
        ref = normed.at[:, pl.ds(pl.multiple_of(owner * half_rows, ROWS), half_rows)]
        return pltpu.make_async_remote_copy(
            src_ref=ref, dst_ref=ref, send_sem=nsem.at[0], recv_sem=nsem.at[1],
            device_id={"tp": 1 - tp}, device_id_type=MESH)

    for p in order:
        for w in (0, 1):
            first_wait(w, p)
            second_all(w, p)
        if p == order[0]:
            launch(normed_copy(tp))
    for w in (2, 3):
        for k in order:
            launch(first(w, k))
    for p in [0] + order:
        for w in (0, 1):
            forward(w, p)
    for w in (2, 3):
        second_all(w, 0)
    for p in [0] + order:
        for w in (0, 1):
            last_wait(w, p)
    for p in order:
        for w in (2, 3):
            first_wait(w, p)
            second_all(w, p)
    for copy in local[1:]:
        copy.wait()
    normed_copy(1 - tp).wait_recv()

    def lanes(c):
        return pl.ds(pl.multiple_of(c * COLS, COLS), COLS)

    def entry_step(i, c):
        s, b = i // nb, lanes(i % nb)
        x = normed[s]
        cbuf[s, HALO:, b] = jnp.dot(x, w0[:, b], preferred_element_type=F32).astype(BF16)
        pbuf[s, HALO:, b] = jnp.dot(x, w1[:, b], preferred_element_type=F32).astype(BF16)
        return c

    lax.fori_loop(0, seqs * nb, entry_step, 0)

    def halo(i, ref):
        return pltpu.make_async_remote_copy(
            src_ref=ref.at[:, rows:], dst_ref=ref.at[:, :HALO], send_sem=hsem_s.at[i],
            recv_sem=hsem_r.at[i], device_id={"sp": (sp + 1) % n}, device_id_type=MESH)

    todo = [(w, p) for p in [0] + order for w in (2, 3)]

    def some_forwards(count):
        for w, p in todo[:count]:
            forward(w, p)
        del todo[:count]

    some_forwards(2)

    @pl.when(sp < n - 1)
    def _():
        halo(0, cbuf).start()
        halo(1, pbuf).start()

    @pl.when(sp > 0)
    def _():
        halo(0, cbuf).wait_recv()
        halo(1, pbuf).wait_recv()

    @pl.when(sp == 0)
    def _():
        cbuf[:, :HALO, :] = jnp.zeros((seqs, HALO, chans), BF16)
        pbuf[:, :HALO, :] = jnp.zeros((seqs, HALO, chans), BF16)

    tap_count = taps.shape[0]
    inverse_length = 1.0 / (rows * n)

    def chain_step(g, s):
        b = lanes(g)
        tap = taps[:, b].astype(F32)

        def conv(i, c):
            r = pl.multiple_of(i * ROWS, ROWS)
            v = cbuf[s, pl.ds(r, ROWS + HALO), b].astype(F32)
            total = v * tap[tap_count - 1 : tap_count]
            for j in range(tap_count - 1):
                total = total + pltpu.roll(v, tap_count - 1 - j, 0) * tap[j : j + 1]
            convb[pl.ds(r, ROWS), :] = total[HALO:].astype(BF16)
            return c

        lax.fori_loop(0, rows // ROWS, conv, 0)
        x = convb[...]
        zr[...] = jnp.dot(x, rg[g], preferred_element_type=F32)
        zi[...] = jnp.dot(x, ig[g], preferred_element_type=F32)
        rate = -RECUR_SCALE * (jnp.exp(dlog[:, b]) * inverse_length)
        row = lax.broadcasted_iota(jnp.int32, (ROWS, COLS), 0)

        def scan(i, carry):
            r = pl.multiple_of(i * ROWS, ROWS)
            at = pl.ds(r, ROWS)
            log_decay = jax.nn.sigmoid(zr[at, :]) * rate + shift[s, at, b]
            a = jnp.exp(log_decay)
            d = (jnp.sqrt(neg_expm1(2.0 * log_decay)) * jax.nn.sigmoid(zi[at, :])
                 * convb[at, :].astype(F32))
            k = 1
            while k < ROWS:
                before = row >= k
                d = d + a * jnp.where(before, pltpu.roll(d, k, 0), 0.0)
                a = a * jnp.where(before, pltpu.roll(a, k, 0), 1.0)
                k *= 2
            d = d + a * carry[1]
            a = a * carry[0]
            cum_a[s, at, b] = a
            cum_b[s, at, b] = d
            return a[ROWS - 1 :], d[ROWS - 1 :]

        end = lax.fori_loop(
            0, rows // ROWS, scan, (jnp.ones((1, COLS), F32), jnp.zeros((1, COLS), F32)))
        my_ab[pl.ds(s, 1), b] = end[0]
        my_ab[pl.ds(seqs + s, 1), b] = end[1]

    for s in range(seqs):
        def chain_group(g, c, s=s):
            chain_step(g, s)
            return c

        for g0 in range(0, nb, 2):
            lax.fori_loop(g0, min(g0 + 2, nb), chain_group, 0)
            some_forwards(max(1, len(todo) // (2 * seqs)))

    def ab_copy(k):
        return pltpu.make_async_remote_copy(
            src_ref=my_ab, dst_ref=all_ab.at[k], send_sem=ab_s.at[k], recv_sem=ab_r.at[k],
            device_id={"sp": (sp + k) % n}, device_id_type=MESH)

    def pool_group(g):
        b = slice(g * COLS, (g + 1) * COLS)
        window = 2 ** (1 + g % 4)

        def diff(i, c):
            s, r = i // (rows // ROWS), pl.multiple_of((i % (rows // ROWS)) * ROWS, ROWS)
            v = pbuf[s, pl.ds(r, ROWS + HALO), b].astype(F32)
            total, k = v, 1
            while k < window:
                total = total + pltpu.roll(total, k, 0)
                k *= 2
            t = lax.broadcasted_iota(jnp.int32, (ROWS, COLS), 0) + (sp * rows + r + 1)
            count = jnp.minimum(t, window).astype(F32)
            convb_pool = total[HALO:] / count - v[HALO:]
            pooled[s, pl.ds(r, ROWS), b] = convb_pool.astype(BF16)
            return c

        lax.fori_loop(0, seqs * (rows // ROWS), diff, 0)
        for s in range(seqs):
            y = jnp.dot(pooled[s, :, b], pm[g], preferred_element_type=F32)
            pooled[s, :, b] = (y * pscale[:, b]).astype(BF16)

    pool_group(0)
    for k in range(1, n):
        @pl.when(sp + k < n)
        def _(k=k):
            ab_copy(k).start()

    for g in range(1, nb):
        pool_group(g)
        some_forwards(1)
    some_forwards(len(todo))

    ent[...] = start[...]
    for k in range(n - 1, 0, -1):
        @pl.when(sp >= k)
        def _(k=k):
            ab_copy(k).wait_recv()
            ent[...] = all_ab[k, :seqs, :] * ent[...] + all_ab[k, seqs : 2 * seqs, :]

    for s in range(seqs):
        def fix(i, c, s=s):
            at = pl.ds(pl.multiple_of(i * ROWS, ROWS), ROWS)
            rec[s, at, :] = (cum_a[s, at, :] * ent[s : s + 1, :] + cum_b[s, at, :]).astype(BF16)
            return c

        lax.fori_loop(0, rows // ROWS, fix, 0)

    for p in [0] + order:
        for w in (2, 3):
            last_wait(w, p)

    out_count = width // COLS
    dims = (((1,), (1,)), ((), ()))

    def partial(owner, j):
        at = pl.ds(pl.multiple_of(owner * half_rows, ROWS), half_rows)
        b = lanes(j)
        x = rec[:, at, :].reshape(seqs * half_rows, chans)
        y = pooled[:, at, :].reshape(seqs * half_rows, chans)
        return lax.dot_general(x, w2[b, :], dims, preferred_element_type=F32) + lax.dot_general(
            y, w3[b, :], dims, preferred_element_type=F32)

    def out_copy(j):
        return pltpu.make_async_remote_copy(
            src_ref=sendbuf.at[j], dst_ref=recvbuf.at[j], send_sem=out_s.at[j],
            recv_sem=out_r.at[j], device_id={"tp": 1 - tp}, device_id_type=MESH)

    def exit_step(j, c):
        sendbuf[j] = partial(1 - tp, j).astype(BF16)
        acc[j] = partial(tp, j)
        out_copy(j).start()
        return c

    lax.fori_loop(0, out_count, exit_step, 0)

    def out_step(j, c):
        out_copy(j).wait_recv()
        total = (acc[j] + recvbuf[j].astype(F32)).astype(BF16)
        out[:, :, lanes(j)] = total.reshape(seqs, half_rows, COLS)
        return c

    lax.fori_loop(0, out_count, out_step, 0)

    def out_end(j, c):
        out_copy(j).wait_send()
        return c

    lax.fori_loop(0, out_count, out_end, 0)
    for copy in started:
        copy.wait_send()

    @pl.when(sp < n - 1)
    def _():
        halo(0, cbuf).wait_send()
        halo(1, pbuf).wait_send()

    for k in range(1, n):
        @pl.when(sp + k < n)
        def _(k=k):
            ab_copy(k).wait_send()


def per_device(n, m, *args):
    (tokens, norm_gain, chain_entry, pool_entry, conv_taps, recur_gate, input_gate, decay_log,
     decay_shift, start_state, pool_mix, pool_scale, chain_exit, pool_exit) = args
    seqs, half_rows, width = tokens.shape
    rows, chans = 2 * half_rows, chain_entry.shape[1]
    nb = chans // COLS
    assert pool_mix.shape[0] % 4 == 0 and pool_mix.shape[1] == COLS
    far = max(m // 2, 1)
    hbm, vmem = pl.BlockSpec(memory_space=pl.ANY), pl.BlockSpec(memory_space=pltpu.VMEM)
    dma = pltpu.SemaphoreType.DMA
    ab_rows = -(-2 * seqs // 8) * 8
    out_count = width // COLS
    scratch = [pltpu.VMEM((width, chans), BF16)] * 4 + [
        pltpu.VMEM((seqs, half_rows, width), BF16),
        pltpu.VMEM((seqs, rows, width), BF16),
        pltpu.VMEM((seqs, HALO + rows, chans), BF16),
        pltpu.VMEM((seqs, HALO + rows, chans), BF16),
        pltpu.VMEM((seqs, rows, chans), F32),
        pltpu.VMEM(recur_gate.shape, BF16),
        pltpu.VMEM(input_gate.shape, BF16),
        pltpu.VMEM(pool_mix.shape, BF16),
        pltpu.VMEM((rows, COLS), BF16),
        pltpu.VMEM((rows, COLS), F32),
        pltpu.VMEM((rows, COLS), F32),
        pltpu.VMEM((seqs, rows, chans), F32),
        pltpu.VMEM((seqs, rows, chans), F32),
        pltpu.VMEM((seqs, rows, chans), BF16),
        pltpu.VMEM((seqs, rows, chans), BF16),
        pltpu.VMEM((ab_rows, chans), F32),
        pltpu.VMEM((n, ab_rows, chans), F32),
        pltpu.VMEM((seqs, chans), F32),
        pltpu.VMEM((out_count, seqs * half_rows, COLS), F32),
        pltpu.VMEM((out_count, seqs * half_rows, COLS), BF16),
        pltpu.VMEM((out_count, seqs * half_rows, COLS), BF16),
        dma((4 * n,)), dma((4 * n,)), dma((8 * n * far,)), dma((8 * n * far,)),
        dma((9,)), dma((2,)), dma((2,)), dma((2,)), dma((n,)), dma((n,)),
        dma((out_count,)), dma((out_count,)),
    ]
    return pl.pallas_call(
        functools.partial(kernel, n, m),
        name="layer",
        out_shape=jax.ShapeDtypeStruct(tokens.shape, BF16),
        in_specs=[hbm, vmem, hbm, hbm, vmem, hbm, hbm, vmem, hbm, vmem, hbm, vmem, hbm, hbm],
        out_specs=vmem,
        scratch_shapes=scratch,
        compiler_params=pltpu.CompilerParams(
            collective_id=0, has_side_effects=True, vmem_limit_bytes=62 * 1024 * 1024),
    )(tokens, norm_gain[None], chain_entry, pool_entry, conv_taps, recur_gate, input_gate,
      decay_log[None], decay_shift, start_state, pool_mix, pool_scale[None],
      chain_exit.T, pool_exit.T)


def solution(mesh):
    in_specs = (
        P("fs", ("sp", "tp"), None),
        P(),
        P(("sp", "fs"), "tp"),
        P(("sp", "fs"), "tp"),
        P(None, "tp"),
        P("tp", None, None),
        P("tp", None, None),
        P("tp"),
        P("fs", "sp", "tp"),
        P("fs", "tp"),
        P("tp", None, None),
        P("tp"),
        P("tp", ("sp", "fs")),
        P("tp", ("sp", "fs")),
    )
    out_specs = P("fs", ("sp", "tp"), None)
    return jax.shard_map(
        functools.partial(per_device, mesh.shape["sp"], mesh.shape["fs"]),
        mesh=mesh, in_specs=in_specs, out_specs=out_specs, check_vma=False)
```

```python
import functools

import jax
import jax.numpy as jnp
from jax import lax
from jax.experimental import pallas as pl
from jax.experimental.pallas import tpu as pltpu
from jax.sharding import PartitionSpec as P

MESH = pl.DeviceIdType.MESH
NORM_EPSILON = 1e-06
RECUR_SCALE = 8.0
HALO = 16
COLS = 256
ROWS = 64
F32 = jnp.float32
BF16 = jnp.bfloat16


def neg_expm1(x):
    y = -x
    poly = 1.0 - y * (1.0 / 9.0)
    for k in range(8, 1, -1):
        poly = 1.0 - y * (1.0 / k) * poly
    return jnp.where(y < 0.5, y * poly, 1.0 - jnp.exp(x))


def kernel(
    n, m,
    tokens, gain, chain_entry, pool_entry, taps, rgate, igate, dlog, shift_hbm, start,
    pmix, pscale, chain_exit, pool_exit,
    out,
    w0, w1, w2, w3, raw, normed, cbuf, pbuf, shift, rg, ig, pm,
    convb, zr, zi, cum_a, cum_b, rec, pooled, my_ab, all_ab, ent, acc, sendbuf, recvbuf,
    s1, r1, s2, r2, t1s, t1r, t2s, t2r, loc, nsem, hsem_s, hsem_r, ab_s, ab_r, out_s, out_r,
):
    sp, fs, tp = lax.axis_index("sp"), lax.axis_index("fs"), lax.axis_index("tp")
    shards = (chain_entry, pool_entry, chain_exit, pool_exit)
    bufs = (w0, w1, w2, w3)
    seqs, half_rows, width = raw.shape
    rows = 2 * half_rows
    chans = cbuf.shape[2]
    nb = chans // COLS
    far = m // 2
    full = (m - 1) // 2

    def ring(i):
        return i + (i // 2) * (5 - 2 * i) if m == 4 else i

    pos = ring(fs)
    right, left = ring((pos + 1) % m), ring((pos + m - 1) % m)

    barrier = pltpu.get_barrier_semaphore()
    greet = [{"sp": (sp + k) % n} for k in range(1, n)] + [{"tp": 1 - tp}]
    greet += [{"fs": ring((pos + k) % m)} for k in range(1, m)]
    for device in greet:
        pl.semaphore_signal(barrier, inc=1, device_id=device, device_id_type=MESH)

    def span(w, part):
        block = shards[w].shape[0]
        tail = block // 8 // 16 * 16
        head = block - tail
        cut = -(-head // 32) * 16
        if w % 2:
            cut = head - cut
        return {"all": (0, block), None: (0, head), 0: (0, cut), 1: (cut, head - cut),
                2: (head, tail)}[part]

    def region(w, p, q, part=None):
        lo, size = span(w, part)
        at = (((sp + p) % n) * m + ring((pos + q + m) % m)) * shards[w].shape[0] + lo
        return bufs[w].at[pl.ds(pl.multiple_of(at, 16), size)]

    def own(w, part=None):
        lo, size = span(w, part)
        return shards[w].at[pl.ds(lo, size)]

    has_tail = span(0, 2)[1] > 0 and m > 1

    started = []

    def launch(copy):
        copy.start()
        started.append(copy)

    def first(w, k):
        return pltpu.make_async_remote_copy(
            src_ref=own(w), dst_ref=region(w, 0, 0), send_sem=s1.at[w * n + k],
            recv_sem=r1.at[w * n + n - k], device_id={"sp": (sp + k) % n}, device_id_type=MESH)

    def first_wait(w, p):
        pltpu.make_async_remote_copy(
            src_ref=own(w), dst_ref=region(w, p, 0), send_sem=s1.at[w * n + p],
            recv_sem=r1.at[w * n + p], device_id={"sp": (sp + p) % n},
            device_id_type=MESH).wait_recv()

    def second(w, p, way, d):
        q = -d if way == 0 else d
        part = way if (m % 2 == 0 and d + 1 == far) else None
        if p == 0 and d == 0:
            src = own(w, part)
        else:
            src = region(w, p, q, part)
        at = ((w * n + p) * 2 + way) * max(far, 1) + d
        return pltpu.make_async_remote_copy(
            src_ref=src, dst_ref=region(w, p, q, part), send_sem=s2.at[at], recv_sem=r2.at[at],
            device_id={"fs": right if way == 0 else left}, device_id_type=MESH)

    def second_wait(w, p, way, d):
        q = -d if way == 0 else d
        part = way if (m % 2 == 0 and d == far) else None
        at = ((w * n + p) * 2 + way) * max(far, 1) + d - 1
        ref = region(w, p, q, part)
        pltpu.make_async_remote_copy(
            src_ref=ref, dst_ref=ref, send_sem=s2.at[at], recv_sem=r2.at[at],
            device_id={"fs": right if way == 0 else left}, device_id_type=MESH).wait_recv()

    def second_all(w, p):
        if far >= 1:
            for way in (0, 1):
                launch(second(w, p, way, 0))

    def forward(w, p):
        for d in range(1, far):
            for way in (0, 1):
                second_wait(w, p, way, d)
                launch(second(w, p, way, d))

    def last_wait(w, p):
        tail_wait(w, p)
        if far >= 1:
            for way in (0, 1):
                second_wait(w, p, way, far)

    def tail_one(w, k):
        return pltpu.make_async_remote_copy(
            src_ref=own(w, 2), dst_ref=region(w, 0, 0, 2), send_sem=t1s.at[w * m + k],
            recv_sem=t1r.at[w * m + m - k], device_id={"fs": ring((pos + k) % m)},
            device_id_type=MESH)

    def tail_one_wait(w, q):
        ref = region(w, 0, q, 2)
        pltpu.make_async_remote_copy(
            src_ref=ref, dst_ref=ref, send_sem=t1s.at[w * m + q], recv_sem=t1r.at[w * m + q],
            device_id={"fs": ring((pos + q) % m)}, device_id_type=MESH).wait_recv()

    def tail_two(w, q, k):
        at = (w * m + q) * n
        return pltpu.make_async_remote_copy(
            src_ref=own(w, 2) if q == 0 else region(w, 0, q, 2), dst_ref=region(w, 0, q, 2),
            send_sem=t2s.at[at + k], recv_sem=t2r.at[at + n - k],
            device_id={"sp": (sp + k) % n}, device_id_type=MESH)

    def tail_start(w):
        if has_tail:
            for k in range(1, m):
                launch(tail_one(w, k))

    def tail_forward(w):
        if has_tail:
            for q in range(m):
                if q:
                    tail_one_wait(w, q)
                for k in order:
                    launch(tail_two(w, q, k))

    def tail_wait(w, p):
        if has_tail and p:
            for q in range(m):
                ref = region(w, p, q, 2)
                at = (w * m + q) * n + p
                pltpu.make_async_remote_copy(
                    src_ref=ref, dst_ref=ref, send_sem=t2s.at[at], recv_sem=t2r.at[at],
                    device_id={"sp": (sp + p) % n}, device_id_type=MESH).wait_recv()

    order = sorted(range(1, n), key=lambda p: min(p, n - p))
    local = [
        pltpu.make_async_copy(tokens, raw, loc.at[0]),
        pltpu.make_async_copy(shift_hbm, shift, loc.at[1]),
        pltpu.make_async_copy(rgate, rg, loc.at[2]),
        pltpu.make_async_copy(igate, ig, loc.at[3]),
        pltpu.make_async_copy(pmix, pm, loc.at[4]),
    ] + [pltpu.make_async_copy(shards[w], region(w, 0, 0, "all"), loc.at[5 + w]) for w in range(4)]
    for copy in local:
        copy.start()

    pl.semaphore_wait(barrier, len(greet))
    for w in (0, 1):
        second_all(w, 0)
        for k in order:
            launch(first(w, k))
        tail_start(w)

    local[0].wait()
    mine = tp * half_rows

    def norm_step(i, c):
        s, r = i // (half_rows // ROWS), (i % (half_rows // ROWS)) * ROWS
        x = raw[s, pl.ds(pl.multiple_of(r, ROWS), ROWS), :].astype(F32)
        scale = lax.rsqrt(jnp.mean(x * x, axis=-1, keepdims=True) + NORM_EPSILON)
        normed[s, pl.ds(pl.multiple_of(mine + r, ROWS), ROWS), :] = (
            x * scale * gain[...]).astype(BF16)
        return c

    lax.fori_loop(0, seqs * (half_rows // ROWS), norm_step, 0)

    def normed_copy(owner):
        ref = normed.at[:, pl.ds(pl.multiple_of(owner * half_rows, ROWS), half_rows)]
        return pltpu.make_async_remote_copy(
            src_ref=ref, dst_ref=ref, send_sem=nsem.at[0], recv_sem=nsem.at[1],
            device_id={"tp": 1 - tp}, device_id_type=MESH)

    for p in order:
        for w in (0, 1):
            first_wait(w, p)
            second_all(w, p)
        if p == order[0]:
            launch(normed_copy(tp))
    for w in (0, 1):
        tail_forward(w)
    for w in (2, 3):
        for k in order:
            launch(first(w, k))
        tail_start(w)
    for p in [0] + order:
        for w in (0, 1):
            forward(w, p)
    for w in (2, 3):
        second_all(w, 0)
    for p in [0] + order:
        for w in (0, 1):
            last_wait(w, p)
    for p in order:
        for w in (2, 3):
            first_wait(w, p)
            second_all(w, p)
    for w in (2, 3):
        tail_forward(w)
    for copy in local[1:]:
        copy.wait()
    normed_copy(1 - tp).wait_recv()

    def lanes(c):
        return pl.ds(pl.multiple_of(c * COLS, COLS), COLS)

    def entry_step(i, c):
        s, b = i // nb, lanes(i % nb)
        x = normed[s]
        cbuf[s, HALO:, b] = jnp.dot(x, w0[:, b], preferred_element_type=F32).astype(BF16)
        pbuf[s, HALO:, b] = jnp.dot(x, w1[:, b], preferred_element_type=F32).astype(BF16)
        return c

    lax.fori_loop(0, seqs * nb, entry_step, 0)

    def halo(i, ref):
        return pltpu.make_async_remote_copy(
            src_ref=ref.at[:, rows:], dst_ref=ref.at[:, :HALO], send_sem=hsem_s.at[i],
            recv_sem=hsem_r.at[i], device_id={"sp": (sp + 1) % n}, device_id_type=MESH)

    todo = [(w, p) for p in [0] + order for w in (2, 3)]

    def some_forwards(count):
        for w, p in todo[:count]:
            forward(w, p)
        del todo[:count]

    some_forwards(2)

    @pl.when(sp < n - 1)
    def _():
        halo(0, cbuf).start()
        halo(1, pbuf).start()

    @pl.when(sp > 0)
    def _():
        halo(0, cbuf).wait_recv()
        halo(1, pbuf).wait_recv()

    @pl.when(sp == 0)
    def _():
        cbuf[:, :HALO, :] = jnp.zeros((seqs, HALO, chans), BF16)
        pbuf[:, :HALO, :] = jnp.zeros((seqs, HALO, chans), BF16)

    tap_count = taps.shape[0]
    inverse_length = 1.0 / (rows * n)

    def chain_step(g, s):
        b = lanes(g)
        tap = taps[:, b].astype(F32)

        def conv(i, c):
            r = pl.multiple_of(i * ROWS, ROWS)
            v = cbuf[s, pl.ds(r, ROWS + HALO), b].astype(F32)
            total = v * tap[tap_count - 1 : tap_count]
            for j in range(tap_count - 1):
                total = total + pltpu.roll(v, tap_count - 1 - j, 0) * tap[j : j + 1]
            convb[pl.ds(r, ROWS), :] = total[HALO:].astype(BF16)
            return c

        lax.fori_loop(0, rows // ROWS, conv, 0)
        x = convb[...]
        zr[...] = jnp.dot(x, rg[g], preferred_element_type=F32)
        zi[...] = jnp.dot(x, ig[g], preferred_element_type=F32)
        rate = -RECUR_SCALE * (jnp.exp(dlog[:, b]) * inverse_length)
        row = lax.broadcasted_iota(jnp.int32, (ROWS, COLS), 0)

        def scan(i, carry):
            r = pl.multiple_of(i * ROWS, ROWS)
            at = pl.ds(r, ROWS)
            log_decay = jax.nn.sigmoid(zr[at, :]) * rate + shift[s, at, b]
            a = jnp.exp(log_decay)
            d = (jnp.sqrt(neg_expm1(2.0 * log_decay)) * jax.nn.sigmoid(zi[at, :])
                 * convb[at, :].astype(F32))
            k = 1
            while k < ROWS:
                before = row >= k
                d = d + a * jnp.where(before, pltpu.roll(d, k, 0), 0.0)
                a = a * jnp.where(before, pltpu.roll(a, k, 0), 1.0)
                k *= 2
            d = d + a * carry[1]
            a = a * carry[0]
            cum_a[s, at, b] = a
            cum_b[s, at, b] = d
            return a[ROWS - 1 :], d[ROWS - 1 :]

        end = lax.fori_loop(
            0, rows // ROWS, scan, (jnp.ones((1, COLS), F32), jnp.zeros((1, COLS), F32)))
        my_ab[pl.ds(s, 1), b] = end[0]
        my_ab[pl.ds(seqs + s, 1), b] = end[1]

    for s in range(seqs):
        def chain_group(g, c, s=s):
            chain_step(g, s)
            return c

        for g0 in range(0, nb, 2):
            lax.fori_loop(g0, min(g0 + 2, nb), chain_group, 0)
            some_forwards(max(1, len(todo) // (2 * seqs)))

    def ab_copy(k):
        return pltpu.make_async_remote_copy(
            src_ref=my_ab, dst_ref=all_ab.at[k], send_sem=ab_s.at[k], recv_sem=ab_r.at[k],
            device_id={"sp": (sp + k) % n}, device_id_type=MESH)

    def pool_group(g):
        b = slice(g * COLS, (g + 1) * COLS)
        window = 2 ** (1 + g % 4)

        def diff(i, c):
            s, r = i // (rows // ROWS), pl.multiple_of((i % (rows // ROWS)) * ROWS, ROWS)
            v = pbuf[s, pl.ds(r, ROWS + HALO), b].astype(F32)
            total, k = v, 1
            while k < window:
                total = total + pltpu.roll(total, k, 0)
                k *= 2
            t = lax.broadcasted_iota(jnp.int32, (ROWS, COLS), 0) + (sp * rows + r + 1)
            count = jnp.minimum(t, window).astype(F32)
            convb_pool = total[HALO:] / count - v[HALO:]
            pooled[s, pl.ds(r, ROWS), b] = convb_pool.astype(BF16)
            return c

        lax.fori_loop(0, seqs * (rows // ROWS), diff, 0)
        for s in range(seqs):
            y = jnp.dot(pooled[s, :, b], pm[g], preferred_element_type=F32)
            pooled[s, :, b] = (y * pscale[:, b]).astype(BF16)

    pool_group(0)
    for k in range(1, n):
        @pl.when(sp + k < n)
        def _(k=k):
            ab_copy(k).start()

    for g in range(1, nb):
        pool_group(g)
        some_forwards(1)
    some_forwards(len(todo))

    ent[...] = start[...]
    for k in range(n - 1, 0, -1):
        @pl.when(sp >= k)
        def _(k=k):
            ab_copy(k).wait_recv()
            ent[...] = all_ab[k, :seqs, :] * ent[...] + all_ab[k, seqs : 2 * seqs, :]

    for s in range(seqs):
        def fix(i, c, s=s):
            at = pl.ds(pl.multiple_of(i * ROWS, ROWS), ROWS)
            rec[s, at, :] = (cum_a[s, at, :] * ent[s : s + 1, :] + cum_b[s, at, :]).astype(BF16)
            return c

        lax.fori_loop(0, rows // ROWS, fix, 0)

    dims = (((1,), (1,)), ((), ()))
    out_cols = sendbuf.shape[2]
    out_count = width // out_cols
    per_group = m * chain_exit.shape[0] // out_cols

    def out_lanes(j):
        return pl.ds(pl.multiple_of(j * out_cols, out_cols), out_cols)

    def partial(owner, j):
        at = pl.ds(pl.multiple_of(owner * half_rows, ROWS), half_rows)
        b = out_lanes(j)
        x = rec[:, at, :].reshape(seqs * half_rows, chans)
        y = pooled[:, at, :].reshape(seqs * half_rows, chans)
        return lax.dot_general(x, w2[b, :], dims, preferred_element_type=F32) + lax.dot_general(
            y, w3[b, :], dims, preferred_element_type=F32)

    def out_copy(j):
        return pltpu.make_async_remote_copy(
            src_ref=sendbuf.at[j], dst_ref=recvbuf.at[j], send_sem=out_s.at[j],
            recv_sem=out_r.at[j], device_id={"tp": 1 - tp}, device_id_type=MESH)

    def exit_step(j, c):
        sendbuf[j] = partial(1 - tp, j).astype(BF16)
        acc[j] = partial(tp, j)
        out_copy(j).start()
        return c

    def out_step(j, c):
        out_copy(j).wait_recv()
        total = (acc[j] + recvbuf[j].astype(F32)).astype(BF16)
        out[:, :, out_lanes(j)] = total.reshape(seqs, half_rows, out_cols)
        return c

    def group(p, step):
        j = ((sp + p) % n) * per_group
        lax.fori_loop(j, j + per_group, step, 0)

    before = None
    for p in [0] + order:
        for w in (2, 3):
            last_wait(w, p)
        group(p, exit_step)
        if before is not None:
            group(before, out_step)
        before = p
    group(before, out_step)

    def out_end(j, c):
        out_copy(j).wait_send()
        return c

    lax.fori_loop(0, out_count, out_end, 0)
    for copy in started:
        copy.wait_send()

    @pl.when(sp < n - 1)
    def _():
        halo(0, cbuf).wait_send()
        halo(1, pbuf).wait_send()

    for k in range(1, n):
        @pl.when(sp + k < n)
        def _(k=k):
            ab_copy(k).wait_send()


def per_device(n, m, *args):
    (tokens, norm_gain, chain_entry, pool_entry, conv_taps, recur_gate, input_gate, decay_log,
     decay_shift, start_state, pool_mix, pool_scale, chain_exit, pool_exit) = args
    seqs, half_rows, width = tokens.shape
    rows, chans = 2 * half_rows, chain_entry.shape[1]
    nb = chans // COLS
    assert pool_mix.shape[0] % 4 == 0 and pool_mix.shape[1] == COLS
    far = max(m // 2, 1)
    hbm, vmem = pl.BlockSpec(memory_space=pl.ANY), pl.BlockSpec(memory_space=pltpu.VMEM)
    dma = pltpu.SemaphoreType.DMA
    ab_rows = -(-2 * seqs // 8) * 8
    out_cols = min(COLS, m * chain_exit.shape[1])
    out_count = width // out_cols
    scratch = [pltpu.VMEM((width, chans), BF16)] * 4 + [
        pltpu.VMEM((seqs, half_rows, width), BF16),
        pltpu.VMEM((seqs, rows, width), BF16),
        pltpu.VMEM((seqs, HALO + rows, chans), BF16),
        pltpu.VMEM((seqs, HALO + rows, chans), BF16),
        pltpu.VMEM((seqs, rows, chans), F32),
        pltpu.VMEM(recur_gate.shape, BF16),
        pltpu.VMEM(input_gate.shape, BF16),
        pltpu.VMEM(pool_mix.shape, BF16),
        pltpu.VMEM((rows, COLS), BF16),
        pltpu.VMEM((rows, COLS), F32),
        pltpu.VMEM((rows, COLS), F32),
        pltpu.VMEM((seqs, rows, chans), F32),
        pltpu.VMEM((seqs, rows, chans), F32),
        pltpu.VMEM((seqs, rows, chans), BF16),
        pltpu.VMEM((seqs, rows, chans), BF16),
        pltpu.VMEM((ab_rows, chans), F32),
        pltpu.VMEM((n, ab_rows, chans), F32),
        pltpu.VMEM((seqs, chans), F32),
        pltpu.VMEM((out_count, seqs * half_rows, out_cols), F32),
        pltpu.VMEM((out_count, seqs * half_rows, out_cols), BF16),
        pltpu.VMEM((out_count, seqs * half_rows, out_cols), BF16),
        dma((4 * n,)), dma((4 * n,)), dma((8 * n * far,)), dma((8 * n * far,)),
        dma((4 * m,)), dma((4 * m,)), dma((4 * m * n,)), dma((4 * m * n,)),
        dma((9,)), dma((2,)), dma((2,)), dma((2,)), dma((n,)), dma((n,)),
        dma((out_count,)), dma((out_count,)),
    ]
    return pl.pallas_call(
        functools.partial(kernel, n, m),
        name="layer",
        out_shape=jax.ShapeDtypeStruct(tokens.shape, BF16),
        in_specs=[hbm, vmem, hbm, hbm, vmem, hbm, hbm, vmem, hbm, vmem, hbm, vmem, hbm, hbm],
        out_specs=vmem,
        scratch_shapes=scratch,
        compiler_params=pltpu.CompilerParams(
            collective_id=0, has_side_effects=True, vmem_limit_bytes=62 * 1024 * 1024),
    )(tokens, norm_gain[None], chain_entry, pool_entry, conv_taps, recur_gate, input_gate,
      decay_log[None], decay_shift, start_state, pool_mix, pool_scale[None],
      chain_exit.T, pool_exit.T)


def solution(mesh):
    in_specs = (
        P("fs", ("sp", "tp"), None),
        P(),
        P(("sp", "fs"), "tp"),
        P(("sp", "fs"), "tp"),
        P(None, "tp"),
        P("tp", None, None),
        P("tp", None, None),
        P("tp"),
        P("fs", "sp", "tp"),
        P("fs", "tp"),
        P("tp", None, None),
        P("tp"),
        P("tp", ("sp", "fs")),
        P("tp", ("sp", "fs")),
    )
    out_specs = P("fs", ("sp", "tp"), None)
    return jax.shard_map(
        functools.partial(per_device, mesh.shape["sp"], mesh.shape["fs"]),
        mesh=mesh, in_specs=in_specs, out_specs=out_specs, check_vma=False)
```
